32 devices in a mesh: sp: 4 (over z), dp: 8 (over y, x, core).
Axes of the slice: x: 2, y: 2, z: 4, core: 2. Of those that a mesh axis runs over, the one named last changes fastest.
Arguments:
- tokens: bfloat16 [8, 768, 2048], P('dp', 'sp'), may hold values from -36 to 36
- query_weight: bfloat16 [2048, 2048], P('dp'), may hold values from -0.125 to 0.125
- key_weight: bfloat16 [2048, 512], P('dp'), may hold values from -0.125 to 0.125
- value_weight: bfloat16 [2048, 512], P('dp'), may hold values from -0.125 to 0.125
- forget_weight: bfloat16 [2048, 16], replicated, may hold values from -0.125 to 0.125
- forget_bias: float32 [16], replicated, may hold values from 3.4 to 9
Outputs:
- mixed: bfloat16 [8, 768, 2048], P('dp', 'sp')
The draws below stay inside these ranges and needn't reach their ends.
All inputs are finite; a program needn't handle non-finite values.
Results may differ from the reference program's by a relative error of at most 0.012.
Values may be sent and summed in bfloat16 or wider, within the bound.
No kernel may reach another device: no remote copies, remote signals or barrier semaphores. Data moves between devices by JAX's collectives and lax.ppermute only.
A program may use at most 64 MiB of HBM per device.

```python
import math
import jax
import jax.numpy as jnp
from jax import lax

D = 2048
H = 16
DH = 128
KV = 4
SEQ = 768
NSEQ = 8


def draw_tokens(key, part):
    base_values = jnp.clip(jax.random.normal(key, (NSEQ, SEQ, D), jnp.float32), -4.0, 4.0)
    return base_values.astype(jnp.bfloat16)


def draw_forget_bias(key, part):
    fast_share = 0.5
    fast_heads = jax.random.uniform(jax.random.fold_in(key, 3), (H,)) < fast_share
    jitter = jax.random.uniform(jax.random.fold_in(key, 5), (H,), jnp.float32)
    return jnp.where(fast_heads, 3.4 + 0.8 * jitter, math.log(SEQ) + 0.4 * jitter).astype(jnp.float32)


def shard_levels(rng, extent, pieces, low, high):
    loudness, own = 1.0, jax.random.fold_in(rng, 6)
    for position, blocks in pieces:
        steps = jnp.exp(jax.random.uniform(jax.random.fold_in(own, position), (blocks,), jnp.float32, low / len(pieces), high / len(pieces)))
        loudness = loudness * jnp.repeat(steps, extent[position] // blocks).reshape([-1 if axis == position else 1 for axis in range(len(extent))])
    return loudness


def centred(key, extent, deviation, reach, shards=(), kind=jnp.bfloat16):
    drawn = deviation * jax.random.normal(key, extent, jnp.float32)
    if shards:
        drawn = drawn * shard_levels(key, extent, shards, -0.22, 0.18)
    return jnp.clip(drawn, -reach, reach).astype(kind)


def setup_inputs(seed: int = 0) -> dict:
    key_list = jax.random.split(jax.random.key(seed), 7)
    return {
        "tokens": draw_tokens(jax.random.fold_in(key_list[6], 71), 0),
        "query_weight": centred(key_list[1], (D, H * DH), D ** -0.5, 0.125, ((0, 8),)),
        "key_weight": centred(key_list[2], (D, KV * DH), D ** -0.5, 0.125, ((0, 8),)),
        "value_weight": centred(key_list[3], (D, KV * DH), D ** -0.5, 0.125, ((0, 8),)),
        "forget_weight": centred(key_list[4], (D, H), D ** -0.5, 0.125),
        "forget_bias": draw_forget_bias(jax.random.fold_in(key_list[6], 71), 0),
    }


def pick_block(length):
    for candidate in (512, 384, 256, 128):
        if length % candidate == 0:
            return candidate
    return length


def reference(tokens, query_weight, key_weight, value_weight, forget_weight, forget_bias):
    seq_count, seq_length, model_width = tokens.shape
    head_count = forget_weight.shape[1]
    head_dim = query_weight.shape[1] // head_count
    key_heads = key_weight.shape[1] // head_dim
    group_size = head_count // key_heads
    token_rows = tokens.reshape(seq_count * seq_length, model_width)
    query_rows = jnp.dot(token_rows, query_weight, preferred_element_type=jnp.float32).astype(jnp.bfloat16)
    query_rows = query_rows.reshape(seq_count, seq_length, head_count, head_dim)
    key_rows = jnp.dot(token_rows, key_weight, preferred_element_type=jnp.float32).astype(jnp.bfloat16)
    key_rows = key_rows.reshape(seq_count, seq_length, key_heads, head_dim)
    value_rows = jnp.dot(token_rows, value_weight, preferred_element_type=jnp.float32).astype(jnp.bfloat16)
    value_rows = value_rows.reshape(seq_count, seq_length, key_heads, head_dim)
    gate_input = jnp.dot(token_rows, forget_weight, preferred_element_type=jnp.float32) + forget_bias[None, :]
    log_gate = jax.nn.log_sigmoid(gate_input).astype(jnp.bfloat16).reshape(seq_count, seq_length, head_count)
    decay_sum = jnp.cumsum(log_gate.astype(jnp.float32), axis=1)
    block_size = pick_block(seq_length)
    block_count = seq_length // block_size
    score_scale = head_dim ** -0.5
    positions = jnp.arange(seq_length, dtype=jnp.int32)
    offsets = jnp.arange(block_size, dtype=jnp.int32)

    def one_block(flat_index):
        seq_index = flat_index // (head_count * block_count)
        head_index = (flat_index // block_count) % head_count
        block_index = flat_index % block_count
        first_row = block_index * block_size
        zero_index = jnp.zeros((), jnp.int32)
        key_index = head_index // group_size
        query_part = lax.dynamic_slice(query_rows, (seq_index, first_row, head_index, zero_index),
                                       (1, block_size, 1, head_dim)).reshape(block_size, head_dim)
        key_part = lax.dynamic_slice(key_rows, (seq_index, zero_index, key_index, zero_index),
                                     (1, seq_length, 1, head_dim)).reshape(seq_length, head_dim)
        value_part = lax.dynamic_slice(value_rows, (seq_index, zero_index, key_index, zero_index),
                                       (1, seq_length, 1, head_dim)).reshape(seq_length, head_dim)
        decay_row = lax.dynamic_slice(decay_sum, (seq_index, zero_index, head_index),
                                      (1, seq_length, 1)).reshape(seq_length)
        query_decay = lax.dynamic_slice_in_dim(decay_row, first_row, block_size)
        raw_scores = jnp.dot(query_part, key_part.T, preferred_element_type=jnp.float32)
        biased = raw_scores * score_scale + query_decay[:, None] - decay_row[None, :]
        allowed = positions[None, :] <= (first_row + offsets)[:, None]
        masked = jnp.where(allowed, biased, -jnp.inf)
        shifted = jnp.exp(masked - jnp.max(masked, axis=-1, keepdims=True))
        weights = (shifted / jnp.sum(shifted, axis=-1, keepdims=True)).astype(jnp.bfloat16)
        return jnp.dot(weights, value_part, preferred_element_type=jnp.float32).astype(jnp.bfloat16)

    flat_blocks = lax.map(one_block, jnp.arange(seq_count * head_count * block_count, dtype=jnp.int32))
    flat_blocks = flat_blocks.reshape(seq_count, head_count, block_count, block_size, head_dim)
    return flat_blocks.transpose(0, 2, 3, 1, 4).reshape(seq_count, seq_length, head_count * head_dim)
```

```python
import functools
import math

import jax
import jax.numpy as jnp
from jax import lax
from jax.experimental import pallas as pl
from jax.experimental.pallas import tpu as pltpu
from jax.sharding import PartitionSpec as P

VMEM_SPEC = pl.BlockSpec(memory_space=pltpu.VMEM)
FAR = 1e30
GATE_ROWS = 16
HEAD_PAD = 8
NT = (((1,), (1,)), ((), ()))


def core_swap(dp_count):
    return [(i, i ^ 1) for i in range(dp_count)]


def first_hop(dp_count):
    return [(i, i ^ (4 if i & 1 else 2)) for i in range(dp_count)]


def second_hop(dp_count):
    return [(i, i ^ (2 if i & 1 else 4)) for i in range(dp_count)]


def chip_sources():
    device = lax.axis_index("dp")
    core = lax.rem(device, 2)
    chip = lax.div(device, 2)
    near = jnp.where(core == 0, 1, 2)
    far = jnp.where(core == 0, 2, 1)
    return core, [chip, chip ^ near, chip ^ far, chip ^ 3]


def shard_columns(chip, core, depth):
    first = pl.multiple_of((chip * 2 + core) * depth, depth)
    second = pl.multiple_of((chip * 2 + 1 - core) * depth, depth)
    return pl.ds(first, depth), pl.ds(second, depth)


def chip_product(x_refs, weight_ref, chip, core):
    depth = weight_ref.shape[0] // 2
    total = None
    for half, columns in enumerate(shard_columns(chip, core, depth)):
        rows = jnp.concatenate([x_ref[:, columns] for x_ref in x_refs], axis=0)
        term = jnp.dot(
            rows, weight_ref[half * depth : (half + 1) * depth, :], preferred_element_type=jnp.float32
        )
        total = term if total is None else total + term
    return total


def kv_kernel(xh_ref, xo_ref, w0_ref, wa_ref, wb_ref, wab_ref, wf_ref, bias_ref, out_ref):
    core, chips = chip_sources()
    rows = xh_ref.shape[0]
    total = None
    for chip, weight_ref in zip(chips, (w0_ref, wa_ref, wb_ref, wab_ref)):
        term = chip_product((xh_ref, xo_ref), weight_ref, chip, core)
        total = term if total is None else total + term
    for n, x_ref in enumerate((xh_ref, xo_ref)):
        out_ref[n, :rows, :] = total[n * rows : (n + 1) * rows].astype(jnp.bfloat16)
        logit = lax.dot_general(wf_ref[...], x_ref[...], NT, preferred_element_type=jnp.float32)
        logit = logit + bias_ref[:, 0:1]
        gate = jnp.minimum(logit, 0.0) - jnp.log1p(jnp.exp(-jnp.abs(logit)))
        pad = out_ref.shape[2] - rows
        wide = jnp.concatenate([gate, jnp.zeros((HEAD_PAD, pad), jnp.float32)], axis=1)
        tall = jnp.concatenate([wide, jnp.zeros_like(wide)], axis=0)
        out_ref[n, rows:, :] = tall.astype(jnp.bfloat16)


def project_kv(xh, xo, weights, wf, bias):
    rows, width = xh.shape[0], weights[0].shape[1]
    flops = 2 * 2 * rows * xh.shape[1] * width
    return pl.pallas_call(
        kv_kernel,
        out_shape=jax.ShapeDtypeStruct((2, rows + GATE_ROWS, width), jnp.bfloat16),
        in_specs=[VMEM_SPEC] * 8,
        out_specs=VMEM_SPEC,
        cost_estimate=pl.CostEstimate(flops=flops, bytes_accessed=2 * xh.size * 2, transcendentals=0),
        name="project_kv",
    )(xh, xo, *weights, wf, bias)


def q_kernel(xa_ref, xb_ref, xc_ref, xd_ref, w0_ref, wa_ref, wb_ref, out_ref):
    core, chips = chip_sources()
    rows = xa_ref.shape[0]
    total = None
    for chip, weight_ref in zip(chips, (w0_ref, wa_ref, wb_ref)):
        term = chip_product((xa_ref, xb_ref, xc_ref, xd_ref), weight_ref, chip, core)
        total = term if total is None else total + term
    for n in range(4):
        out_ref[n] = total[n * rows : (n + 1) * rows]


def project_q(xs, weights):
    rows, width = xs[0].shape[0], weights[0].shape[1]
    flops = 2 * 4 * rows * 3 * weights[0].shape[0] * width
    return pl.pallas_call(
        q_kernel,
        out_shape=jax.ShapeDtypeStruct((4, rows, width), jnp.float32),
        in_specs=[VMEM_SPEC] * 7,
        out_specs=VMEM_SPEC,
        cost_estimate=pl.CostEstimate(flops=flops, bytes_accessed=4 * xs[0].size * 2, transcendentals=0),
        name="project_q",
    )(*xs, *weights)


def attend_kernel(
    partner, scale, acc_ref, xh_ref, xo_ref, w_ref, own_ref, par_ref, lown_ref, lpar_ref, outh_ref, outo_ref
):
    core, chips = chip_sources()
    place = lax.axis_index("sp")
    late = lax.rem(place, 2) == 1
    upper = place >= 2
    rows = xh_ref.shape[0]
    head_dim = own_ref.shape[2] // 2
    heads = w_ref.shape[1] // head_dim
    log2e = math.log2(math.e)
    above = lax.broadcasted_iota(jnp.int32, (rows, rows), 0) <= lax.broadcasted_iota(
        jnp.int32, (rows, rows), 1
    )
    below = lax.broadcasted_iota(jnp.int32, (rows, rows), 0) >= lax.broadcasted_iota(
        jnp.int32, (rows, rows), 1
    )
    upto = jnp.where(above, 1.0, 0.0).astype(jnp.bfloat16)
    last = chip_product((xh_ref, xo_ref), w_ref, chips[3], core)
    other_first = late if not partner else jnp.logical_not(late)
    ones = jnp.ones((rows, head_dim), jnp.bfloat16)
    base_slot = 2 if partner else 0
    for n, out_ref in enumerate((outh_ref, outo_ref)):
        query = (acc_ref[base_slot + n] + last[n * rows : (n + 1) * rows]).astype(jnp.bfloat16)
        self_ref, other_ref = (par_ref, own_ref) if partner else (own_ref, par_ref)
        sums = []
        for ref in (lown_ref, lpar_ref, self_ref, other_ref):
            gates = ref[n, rows : rows + HEAD_PAD, :rows]
            sums.append(jnp.dot(gates, upto, preferred_element_type=jnp.float32))
        ends = [s[:, rows - 1 : rows] for s in sums]
        zero = jnp.zeros_like(ends[0])
        low_total = ends[0] + ends[1]
        bases = [
            jnp.where(late, ends[1], zero),
            jnp.where(late, zero, ends[0]),
            low_total + jnp.where(other_first, ends[3], zero),
            low_total + jnp.where(other_first, zero, ends[2]),
        ]
        decay = [s + b for s, b in zip(sums, bases)]
        query_decay = jnp.transpose(decay[2])
        shown = (upper, upper, None, other_first)
        key_decay = [
            d * log2e if ok is None else jnp.where(ok, d * log2e, FAR) for d, ok in zip(decay, shown)
        ]
        blocks = (lown_ref, lpar_ref, self_ref, other_ref)
        keys = jnp.concatenate([ref[n, :rows, :head_dim] for ref in blocks], axis=0)
        values = jnp.concatenate(
            [jnp.concatenate([ref[n, :rows, head_dim:], ones], axis=1) for ref in blocks], axis=0
        )
        for head in range(heads):
            part = query[:, head * head_dim : (head + 1) * head_dim]
            raw = lax.dot_general(part, keys, NT, preferred_element_type=jnp.float32)
            pieces = []
            for i in range(4):
                piece = raw[:, i * rows : (i + 1) * rows] * (scale * log2e) - key_decay[i][head : head + 1, :]
                if i == 2:
                    piece = jnp.where(below, piece, -FAR)
                pieces.append(piece)
            top = jnp.maximum(jnp.maximum(pieces[0], pieces[1]), jnp.maximum(pieces[2], pieces[3]))
            own_decay = query_decay[:, head : head + 1] * log2e
            row_max = jnp.max(top, axis=1, keepdims=True) + own_decay
            shift = own_decay - row_max
            weight = jnp.concatenate(
                [jnp.exp2(piece + shift).astype(jnp.bfloat16) for piece in pieces], axis=1
            )
            sums_out = jnp.dot(weight, values, preferred_element_type=jnp.float32)
            mixed = sums_out[:, :head_dim] / sums_out[:, head_dim:]
            out_ref[:, head * head_dim : (head + 1) * head_dim] = mixed.astype(jnp.bfloat16)


def attend(partner, scale, acc, xh, xo, weight, blocks):
    rows, width = xh.shape[0], weight.shape[1]
    piece = jax.ShapeDtypeStruct((rows, width), jnp.bfloat16)
    flops = 2 * 2 * rows * 4 * rows * width * 2
    return pl.pallas_call(
        functools.partial(attend_kernel, partner, scale),
        out_shape=(piece, piece),
        in_specs=[VMEM_SPEC] * 8,
        out_specs=(VMEM_SPEC, VMEM_SPEC),
        cost_estimate=pl.CostEstimate(flops=flops, bytes_accessed=acc.size * 4, transcendentals=0),
        name="attend_partner" if partner else "attend_own",
    )(acc, xh, xo, weight, *blocks)


def place_kernel(a_ref, b_ref, c_ref, d_ref, out_ref):
    core = lax.rem(lax.axis_index("dp"), 2)
    half = lax.rem(lax.axis_index("sp"), 2)
    width = a_ref.shape[1]
    groups = (2 * half + core, 2 * half + 1 - core, 2 - 2 * half + core, 3 - 2 * half - core)
    for ref, group in zip((a_ref, b_ref, c_ref, d_ref), groups):
        out_ref[:, pl.ds(pl.multiple_of(group * width, width), width)] = ref[...]


def place(pieces):
    rows, width = pieces[0].shape
    return pl.pallas_call(
        place_kernel,
        out_shape=jax.ShapeDtypeStruct((rows, 4 * width), jnp.bfloat16),
        in_specs=[VMEM_SPEC] * 4,
        out_specs=VMEM_SPEC,
        name="place",
    )(*pieces)


def paired(tokens, query_weight, key_weight, value_weight, forget_weight, forget_bias):
    own_home = tokens[0]
    dp_count, sp_count = lax.axis_size("dp"), lax.axis_size("sp")
    head_count = forget_weight.shape[1]
    head_dim = query_weight.shape[1] // head_count
    group_width = query_weight.shape[1] // sp_count
    group_heads = head_count // sp_count
    core = lax.rem(lax.axis_index("dp"), 2)
    half = lax.rem(lax.axis_index("sp"), 2)
    swap, hop, turn = core_swap(dp_count), first_hop(dp_count), second_hop(dp_count)
    partner = [(i, i ^ 1) for i in range(sp_count)]
    upward = [(i, i + 2) for i in range(sp_count - 2)]
    across = [
        (s * dp_count + d, (s ^ 1) * dp_count + (d ^ 1)) for s in range(sp_count) for d in range(dp_count)
    ]

    def cut(weight, group, width):
        return lax.dynamic_slice_in_dim(weight, group * width, width, 1)

    def cut_kv(group):
        return jnp.concatenate(
            [cut(key_weight, group, head_dim), cut(value_weight, group, head_dim)], axis=1
        )

    mine, other = 2 * half + core, 2 * half + 1 - core
    par_home = lax.ppermute(own_home, "sp", partner)
    kv_0 = jnp.concatenate([cut_kv(mine), lax.ppermute(cut_kv(other), "dp", swap)], axis=0)
    kv_a = lax.ppermute(kv_0, "dp", hop)
    kv_b = lax.ppermute(kv_0, "dp", turn)
    kv_ab = lax.ppermute(kv_a, "dp", turn)
    q_0 = jnp.concatenate(
        [
            cut(query_weight, mine, group_width),
            lax.ppermute(cut(query_weight, other, group_width), "dp", swap),
        ],
        axis=0,
    )
    q_a = lax.ppermute(q_0, "dp", hop)
    q_b = lax.ppermute(q_0, "dp", turn)
    q_ab = lax.ppermute(q_a, "dp", turn)
    own_other = lax.ppermute(own_home, "dp", swap)
    par_other = lax.ppermute(par_home, "dp", swap)

    gate_weight = lax.dynamic_slice_in_dim(forget_weight.T, mine * group_heads, group_heads, 0)
    gate_weight = jnp.pad(gate_weight, ((0, HEAD_PAD - group_heads), (0, 0)))
    gate_bias = lax.dynamic_slice_in_dim(forget_bias, mine * group_heads, group_heads, 0)
    gate_bias = jnp.broadcast_to(
        jnp.pad(gate_bias, (0, HEAD_PAD - group_heads))[:, None], (HEAD_PAD, 128)
    )

    kv_weights = (kv_0, kv_a, kv_b, kv_ab)
    kv_own = project_kv(own_home, own_other, kv_weights, gate_weight, gate_bias)
    low_own = lax.ppermute(kv_own, "sp", upward)
    kv_par = project_kv(par_home, par_other, kv_weights, gate_weight, gate_bias)
    low_par = lax.ppermute(kv_par, "sp", upward)
    partial = project_q((own_home, own_other, par_home, par_other), (q_0, q_a, q_b))
    blocks = (kv_own, kv_par, low_own, low_par)
    scale = head_dim ** (-0.5)
    out_par_home, out_par_other = attend(True, scale, partial, par_home, par_other, q_ab, blocks)
    from_across = lax.ppermute(out_par_other, ("sp", "dp"), across)
    from_partner = lax.ppermute(out_par_home, "sp", partner)
    out_home, out_other = attend(False, scale, partial, own_home, own_other, q_ab, blocks)
    from_core = lax.ppermute(out_other, "dp", swap)
    return place((out_home, from_core, from_partner, from_across))[None]


def pick_block(length):
    for candidate in (512, 384, 256, 128):
        if length % candidate == 0:
            return candidate
    return length


def exchanged(tokens, query_weight, key_weight, value_weight, forget_weight, forget_bias):
    token_rows = tokens[0]
    row_count = token_rows.shape[0]
    sp_count = lax.axis_size("sp")
    head_count = forget_weight.shape[1]
    query_width = query_weight.shape[1]
    key_width = key_weight.shape[1]
    head_dim = query_width // head_count
    key_heads = key_width // head_dim
    pieces = (
        lax.all_gather(query_weight, "dp", axis=0, tiled=True),
        lax.all_gather(key_weight, "dp", axis=0, tiled=True),
        lax.all_gather(value_weight, "dp", axis=0, tiled=True),
    )
    query_rows, key_rows, value_rows = tuple(
        (
            jnp.dot(token_rows, weight_piece, preferred_element_type=jnp.float32)
            for weight_piece in pieces
        )
    )
    query_rows = query_rows.astype(jnp.bfloat16)
    key_rows = key_rows.astype(jnp.bfloat16)
    value_rows = value_rows.astype(jnp.bfloat16)
    gate_input = (
        jnp.dot(token_rows, forget_weight, preferred_element_type=jnp.float32)
        + forget_bias[None, :]
    )
    log_gate = jax.nn.log_sigmoid(gate_input).astype(jnp.bfloat16)
    repeats = max(1, sp_count // key_heads)
    if repeats > 1:
        key_rows = jnp.repeat(key_rows.reshape(row_count, key_heads, head_dim), repeats, axis=1)
        key_rows = key_rows.reshape(row_count, key_heads * repeats * head_dim)
        value_rows = jnp.repeat(value_rows.reshape(row_count, key_heads, head_dim), repeats, axis=1)
        value_rows = value_rows.reshape(row_count, key_heads * repeats * head_dim)
    head_query, head_keys, head_values, head_gates = (
        lax.all_to_all(query_rows, "sp", split_axis=1, concat_axis=0, tiled=True),
        lax.all_to_all(key_rows, "sp", split_axis=1, concat_axis=0, tiled=True),
        lax.all_to_all(value_rows, "sp", split_axis=1, concat_axis=0, tiled=True),
        lax.all_to_all(log_gate, "sp", split_axis=1, concat_axis=0, tiled=True),
    )
    seq_length = head_query.shape[0]
    local_heads = head_count // sp_count
    local_keys = head_keys.shape[1] // head_dim
    group_share = local_heads // local_keys
    decay_sum = jnp.cumsum(head_gates.astype(jnp.float32), axis=0)
    decay_grid = decay_sum.T.reshape(local_keys, group_share, seq_length)
    grouped = head_query.reshape(seq_length, local_keys, group_share, head_dim)
    key_grid = head_keys.reshape(seq_length, local_keys, head_dim)
    value_grid = head_values.reshape(seq_length, local_keys, head_dim)
    block_size = pick_block(seq_length)
    block_count = seq_length // block_size
    score_scale = head_dim ** (-0.5)
    offsets = jnp.arange(block_size, dtype=jnp.int32)

    def query_block(block_index):
        first_row = block_index * block_size
        query_part = lax.dynamic_slice_in_dim(grouped, first_row, block_size, 0)
        query_decay = lax.dynamic_slice_in_dim(decay_grid, first_row, block_size, 2)

        def fill_scores(key_block, buffer):
            key_first = key_block * block_size
            key_part = lax.dynamic_slice_in_dim(key_grid, key_first, block_size, 0)
            key_decay = lax.dynamic_slice_in_dim(decay_grid, key_first, block_size, 2)
            raw_scores = jnp.einsum(
                "qkgd,skd->kgqs", query_part, key_part, preferred_element_type=jnp.float32
            )
            biased = raw_scores * score_scale + query_decay[..., :, None] - key_decay[..., None, :]
            allowed = (key_first + offsets)[None, :] <= (first_row + offsets)[:, None]
            masked = jnp.where(allowed, biased, -jnp.inf)
            return lax.dynamic_update_index_in_dim(buffer, masked, key_block, 0)

        score_buffer = lax.fori_loop(
            0,
            block_index + 1,
            fill_scores,
            jnp.full(
                (block_count, local_keys, group_share, block_size, block_size),
                -jnp.inf,
                jnp.float32,
            ),
        )
        row_max = jnp.max(jnp.max(score_buffer, axis=-1), axis=0)
        row_sum = jnp.sum(
            jnp.sum(jnp.exp(score_buffer - row_max[None, ..., None]), axis=-1), axis=0
        )

        def weighted(key_block, accumulated):
            block_scores = lax.dynamic_index_in_dim(score_buffer, key_block, 0, keepdims=False)
            weights = (jnp.exp(block_scores - row_max[..., None]) / row_sum[..., None]).astype(
                jnp.bfloat16
            )
            value_part = lax.dynamic_slice_in_dim(value_grid, key_block * block_size, block_size, 0)
            return accumulated + jnp.einsum(
                "kgqs,skd->qkgd", weights, value_part, preferred_element_type=jnp.float32
            )

        mixed_block = lax.fori_loop(
            0,
            block_index + 1,
            weighted,
            jnp.zeros((block_size, local_keys, group_share, head_dim), jnp.float32),
        )
        return mixed_block.astype(jnp.bfloat16).reshape(block_size, local_heads * head_dim)

    head_mixed = lax.map(query_block, jnp.arange(block_count, dtype=jnp.int32))
    head_mixed = head_mixed.reshape(seq_length, local_heads * head_dim)
    mixed = lax.all_to_all(head_mixed, "sp", split_axis=0, concat_axis=1, tiled=True)
    return mixed[None]


def on_device(*arrays):
    key_heads = arrays[2].shape[1] * arrays[4].shape[1] // arrays[1].shape[1]
    if lax.axis_size("dp") == 8 and lax.axis_size("sp") == 4 and key_heads == 4:
        return paired(*arrays)
    return exchanged(*arrays)


def solution(mesh):
    placed = (P("dp", "sp", None), P("dp", None), P("dp", None), P("dp", None), P(), P())
    return jax.shard_map(
        on_device, mesh=mesh, in_specs=placed, out_specs=P("dp", "sp", None), check_vma=False
    )
```

```python
import functools
import math

import jax
import jax.numpy as jnp
from jax import lax
from jax.experimental import pallas as pl
from jax.experimental.pallas import tpu as pltpu
from jax.sharding import PartitionSpec as P


VMEM_SPEC = pl.BlockSpec(memory_space=pltpu.VMEM)
KEEP_ROOM = pltpu.CompilerParams(vmem_limit_bytes=24 * 1024 * 1024)
FAR = 1e30
GATE_ROWS = 16
HEAD_PAD = 8
NT = (((1,), (1,)), ((), ()))


def core_swap(dp_count):
    return [(i, i ^ 1) for i in range(dp_count)]


def first_hop(dp_count):
    return [(i, i ^ (4 if i & 1 else 2)) for i in range(dp_count)]


def second_hop(dp_count):
    return [(i, i ^ (2 if i & 1 else 4)) for i in range(dp_count)]


def chip_sources():
    device = lax.axis_index("dp")
    core = lax.rem(device, 2)
    chip = lax.div(device, 2)
    near = jnp.where(core == 0, 1, 2)
    far = jnp.where(core == 0, 2, 1)
    return core, [chip, chip ^ near, chip ^ far, chip ^ 3]


def shard_columns(chip, core, depth):
    first = pl.multiple_of((chip * 2 + core) * depth, depth)
    second = pl.multiple_of((chip * 2 + 1 - core) * depth, depth)
    return pl.ds(first, depth), pl.ds(second, depth)


def chip_product(x_refs, weight_ref, chip, core):
    depth = weight_ref.shape[0] // 2
    total = None
    for half, columns in enumerate(shard_columns(chip, core, depth)):
        rows = jnp.concatenate([x_ref[:, columns] for x_ref in x_refs], axis=0)
        term = jnp.dot(
            rows, weight_ref[half * depth : (half + 1) * depth, :], preferred_element_type=jnp.float32
        )
        total = term if total is None else total + term
    return total


def group_rows(stacked, group, size):
    parts = [
        jnp.concatenate([stacked[i * size : (i + 1) * size]] * (HEAD_PAD // size), axis=0)
        for i in range(stacked.shape[0] // size)
    ]
    chosen = parts[0]
    for i, part in enumerate(parts[1:], 1):
        chosen = jnp.where(group == i, part, chosen)
    return chosen


def kv_kernel(xh_ref, xo_ref, w0_ref, wa_ref, wb_ref, wab_ref, wf_ref, bias_ref, out_ref):
    core, chips = chip_sources()
    group = 2 * lax.rem(lax.axis_index("sp"), 2) + core
    rows = xh_ref.shape[0]
    group_heads = wf_ref.shape[0] // 4
    head_row = lax.broadcasted_iota(jnp.int32, (HEAD_PAD, rows), 0)
    bias = jnp.zeros((HEAD_PAD, rows), jnp.float32)
    for i in range(group_heads):
        bias = jnp.where(head_row == i, bias_ref[group * group_heads + i], bias)
    total = None
    for chip, weight_ref in zip(chips, (w0_ref, wa_ref, wb_ref, wab_ref)):
        term = chip_product((xh_ref, xo_ref), weight_ref, chip, core)
        total = term if total is None else total + term
    for n, x_ref in enumerate((xh_ref, xo_ref)):
        out_ref[n, :rows, :] = total[n * rows : (n + 1) * rows].astype(jnp.bfloat16)
        logit = lax.dot_general(wf_ref[...], x_ref[...], NT, preferred_element_type=jnp.float32)
        logit = group_rows(logit, group, group_heads) + bias
        gate = jnp.minimum(logit, 0.0) - jnp.log1p(jnp.exp(-jnp.abs(logit)))
        pad = out_ref.shape[2] - rows
        wide = jnp.concatenate([gate, jnp.zeros((HEAD_PAD, pad), jnp.float32)], axis=1)
        tall = jnp.concatenate([wide, jnp.zeros_like(wide)], axis=0)
        out_ref[n, rows:, :] = tall.astype(jnp.bfloat16)


def project_kv(xh, xo, weights, wf, bias):
    rows, width = xh.shape[0], weights[0].shape[1]
    flops = 2 * 2 * rows * xh.shape[1] * width
    return pl.pallas_call(
        kv_kernel,
        out_shape=jax.ShapeDtypeStruct((2, rows + GATE_ROWS, width), jnp.bfloat16),
        in_specs=[VMEM_SPEC] * 7 + [pl.BlockSpec(memory_space=pltpu.SMEM)],
        out_specs=VMEM_SPEC,
        cost_estimate=pl.CostEstimate(flops=flops, bytes_accessed=2 * xh.size * 2, transcendentals=0),
        compiler_params=KEEP_ROOM,
        name="project_kv",
    )(xh, xo, *weights, wf, bias)


def q_kernel(xa_ref, xb_ref, xc_ref, xd_ref, w0_ref, wa_ref, wb_ref, out_ref):
    core, chips = chip_sources()
    rows = xa_ref.shape[0]
    total = None
    for chip, weight_ref in zip(chips, (w0_ref, wa_ref, wb_ref)):
        term = chip_product((xa_ref, xb_ref, xc_ref, xd_ref), weight_ref, chip, core)
        total = term if total is None else total + term
    for n in range(4):
        out_ref[n] = total[n * rows : (n + 1) * rows]


def project_q(xs, weights):
    rows, width = xs[0].shape[0], weights[0].shape[1]
    flops = 2 * 4 * rows * 3 * weights[0].shape[0] * width
    return pl.pallas_call(
        q_kernel,
        out_shape=jax.ShapeDtypeStruct((4, rows, width), jnp.float32),
        in_specs=[VMEM_SPEC] * 7,
        out_specs=VMEM_SPEC,
        cost_estimate=pl.CostEstimate(flops=flops, bytes_accessed=4 * xs[0].size * 2, transcendentals=0),
        compiler_params=KEEP_ROOM,
        name="project_q",
    )(*xs, *weights)


def attend_kernel(
    partner, scale, acc_ref, xh_ref, xo_ref, w_ref, own_ref, par_ref, lown_ref, lpar_ref, outh_ref, outo_ref
):
    core, chips = chip_sources()
    place = lax.axis_index("sp")
    late = lax.rem(place, 2) == 1
    upper = place >= 2
    rows = xh_ref.shape[0]
    head_dim = own_ref.shape[2] // 2
    heads = w_ref.shape[1] // head_dim
    log2e = math.log2(math.e)
    above = lax.broadcasted_iota(jnp.int32, (rows, rows), 0) <= lax.broadcasted_iota(
        jnp.int32, (rows, rows), 1
    )
    below = lax.broadcasted_iota(jnp.int32, (rows, rows), 0) >= lax.broadcasted_iota(
        jnp.int32, (rows, rows), 1
    )
    upto = jnp.where(above, 1.0, 0.0).astype(jnp.bfloat16)
    last = chip_product((xh_ref, xo_ref), w_ref, chips[3], core)
    other_first = late if not partner else jnp.logical_not(late)
    ones = jnp.ones((rows, head_dim), jnp.bfloat16)
    base_slot = 2 if partner else 0
    for n, out_ref in enumerate((outh_ref, outo_ref)):
        query = (acc_ref[base_slot + n] + last[n * rows : (n + 1) * rows]).astype(jnp.bfloat16)
        self_ref, other_ref = (par_ref, own_ref) if partner else (own_ref, par_ref)
        sums = []
        for ref in (lown_ref, lpar_ref, self_ref, other_ref):
            gates = ref[n, rows : rows + HEAD_PAD, :rows]
            sums.append(jnp.dot(gates, upto, preferred_element_type=jnp.float32))
        ends = [s[:, rows - 1 : rows] for s in sums]
        zero = jnp.zeros_like(ends[0])
        low_total = ends[0] + ends[1]
        bases = [
            jnp.where(late, ends[1], zero),
            jnp.where(late, zero, ends[0]),
            low_total + jnp.where(other_first, ends[3], zero),
            low_total + jnp.where(other_first, zero, ends[2]),
        ]
        decay = [s + b for s, b in zip(sums, bases)]
        query_decay = jnp.transpose(decay[2])
        shown = (upper, upper, None, other_first)
        key_decay = [
            d * log2e if ok is None else jnp.where(ok, d * log2e, FAR) for d, ok in zip(decay, shown)
        ]
        blocks = (lown_ref, lpar_ref, self_ref, other_ref)
        keys = jnp.concatenate([ref[n, :rows, :head_dim] for ref in blocks], axis=0)
        values = jnp.concatenate(
            [jnp.concatenate([ref[n, :rows, head_dim:], ones], axis=1) for ref in blocks], axis=0
        )
        for head in range(heads):
            part = query[:, head * head_dim : (head + 1) * head_dim]
            raw = lax.dot_general(part, keys, NT, preferred_element_type=jnp.float32)
            pieces = []
            for i in range(4):
                piece = raw[:, i * rows : (i + 1) * rows] * (scale * log2e) - key_decay[i][head : head + 1, :]
                if i == 2:
                    piece = jnp.where(below, piece, -FAR)
                pieces.append(piece)
            top = jnp.maximum(jnp.maximum(pieces[0], pieces[1]), jnp.maximum(pieces[2], pieces[3]))
            own_decay = query_decay[:, head : head + 1] * log2e
            row_max = jnp.max(top, axis=1, keepdims=True) + own_decay
            shift = own_decay - row_max
            weight = jnp.concatenate(
                [jnp.exp2(piece + shift).astype(jnp.bfloat16) for piece in pieces], axis=1
            )
            sums_out = jnp.dot(weight, values, preferred_element_type=jnp.float32)
            mixed = sums_out[:, :head_dim] / sums_out[:, head_dim:]
            out_ref[:, head * head_dim : (head + 1) * head_dim] = mixed.astype(jnp.bfloat16)


def attend(partner, scale, acc, xh, xo, weight, blocks):
    rows, width = xh.shape[0], weight.shape[1]
    piece = jax.ShapeDtypeStruct((rows, width), jnp.bfloat16)
    flops = 2 * 2 * rows * 4 * rows * width * 2
    return pl.pallas_call(
        functools.partial(attend_kernel, partner, scale),
        out_shape=(piece, piece),
        in_specs=[VMEM_SPEC] * 8,
        out_specs=(VMEM_SPEC, VMEM_SPEC),
        cost_estimate=pl.CostEstimate(flops=flops, bytes_accessed=acc.size * 4, transcendentals=0),
        compiler_params=KEEP_ROOM,
        name="attend_partner" if partner else "attend_own",
    )(acc, xh, xo, weight, *blocks)


def place_kernel(a_ref, b_ref, c_ref, d_ref, out_ref):
    core = lax.rem(lax.axis_index("dp"), 2)
    half = lax.rem(lax.axis_index("sp"), 2)
    width = a_ref.shape[1]
    groups = (2 * half + core, 2 * half + 1 - core, 2 - 2 * half + core, 3 - 2 * half - core)
    for ref, group in zip((a_ref, b_ref, c_ref, d_ref), groups):
        out_ref[:, pl.ds(pl.multiple_of(group * width, width), width)] = ref[...]


def place(pieces):
    rows, width = pieces[0].shape
    return pl.pallas_call(
        place_kernel,
        out_shape=jax.ShapeDtypeStruct((rows, 4 * width), jnp.bfloat16),
        in_specs=[VMEM_SPEC] * 4,
        out_specs=VMEM_SPEC,
        compiler_params=KEEP_ROOM,
        name="place",
    )(*pieces)


def paired(tokens, query_weight, key_weight, value_weight, forget_weight, forget_bias):
    own_home = tokens[0]
    dp_count, sp_count = lax.axis_size("dp"), lax.axis_size("sp")
    head_count = forget_weight.shape[1]
    head_dim = query_weight.shape[1] // head_count
    group_width = query_weight.shape[1] // sp_count
    core = lax.rem(lax.axis_index("dp"), 2)
    half = lax.rem(lax.axis_index("sp"), 2)
    swap, hop, turn = core_swap(dp_count), first_hop(dp_count), second_hop(dp_count)
    partner = [(i, i ^ 1) for i in range(sp_count)]
    upward = [(i, i + 2) for i in range(sp_count - 2)]
    across = [
        (s * dp_count + d, (s ^ 1) * dp_count + (d ^ 1)) for s in range(sp_count) for d in range(dp_count)
    ]

    def cut(weight, group, width):
        return lax.dynamic_slice_in_dim(weight, group * width, width, 1)

    def cut_kv(group):
        return jnp.concatenate(
            [cut(key_weight, group, head_dim), cut(value_weight, group, head_dim)], axis=1
        )

    mine, other = 2 * half + core, 2 * half + 1 - core
    par_home = lax.ppermute(own_home, "sp", partner)
    kv_0 = jnp.concatenate([cut_kv(mine), lax.ppermute(cut_kv(other), "dp", swap)], axis=0)
    kv_a = lax.ppermute(kv_0, "dp", hop)
    kv_b = lax.ppermute(kv_0, "dp", turn)
    kv_ab = lax.ppermute(kv_a, "dp", turn)
    q_0 = jnp.concatenate(
        [
            cut(query_weight, mine, group_width),
            lax.ppermute(cut(query_weight, other, group_width), "dp", swap),
        ],
        axis=0,
    )
    q_a = lax.ppermute(q_0, "dp", hop)
    q_b = lax.ppermute(q_0, "dp", turn)
    q_ab = lax.ppermute(q_a, "dp", turn)
    own_other = lax.ppermute(own_home, "dp", swap)
    par_other = lax.ppermute(par_home, "dp", swap)

    kv_weights = (kv_0, kv_a, kv_b, kv_ab)
    kv_own = project_kv(own_home, own_other, kv_weights, forget_weight.T, forget_bias)
    low_own = lax.ppermute(kv_own, "sp", upward)
    kv_par = project_kv(par_home, par_other, kv_weights, forget_weight.T, forget_bias)
    low_par = lax.ppermute(kv_par, "sp", upward)
    partial = project_q((own_home, own_other, par_home, par_other), (q_0, q_a, q_b))
    blocks = (kv_own, kv_par, low_own, low_par)
    scale = head_dim ** (-0.5)
    out_par_home, out_par_other = attend(True, scale, partial, par_home, par_other, q_ab, blocks)
    from_across = lax.ppermute(out_par_other, ("sp", "dp"), across)
    from_partner = lax.ppermute(out_par_home, "sp", partner)
    out_home, out_other = attend(False, scale, partial, own_home, own_other, q_ab, blocks)
    from_core = lax.ppermute(out_other, "dp", swap)
    return place((out_home, from_core, from_partner, from_across))[None]


def pick_block(length):
    for candidate in (512, 384, 256, 128):
        if length % candidate == 0:
            return candidate
    return length


def exchanged(tokens, query_weight, key_weight, value_weight, forget_weight, forget_bias):
    token_rows = tokens[0]
    row_count = token_rows.shape[0]
    sp_count = lax.axis_size("sp")
    head_count = forget_weight.shape[1]
    query_width = query_weight.shape[1]
    key_width = key_weight.shape[1]
    head_dim = query_width // head_count
    key_heads = key_width // head_dim
    pieces = (
        lax.all_gather(query_weight, "dp", axis=0, tiled=True),
        lax.all_gather(key_weight, "dp", axis=0, tiled=True),
        lax.all_gather(value_weight, "dp", axis=0, tiled=True),
    )
    query_rows, key_rows, value_rows = tuple(
        (
            jnp.dot(token_rows, weight_piece, preferred_element_type=jnp.float32)
            for weight_piece in pieces
        )
    )
    query_rows = query_rows.astype(jnp.bfloat16)
    key_rows = key_rows.astype(jnp.bfloat16)
    value_rows = value_rows.astype(jnp.bfloat16)
    gate_input = (
        jnp.dot(token_rows, forget_weight, preferred_element_type=jnp.float32)
        + forget_bias[None, :]
    )
    log_gate = jax.nn.log_sigmoid(gate_input).astype(jnp.bfloat16)
    repeats = max(1, sp_count // key_heads)
    if repeats > 1:
        key_rows = jnp.repeat(key_rows.reshape(row_count, key_heads, head_dim), repeats, axis=1)
        key_rows = key_rows.reshape(row_count, key_heads * repeats * head_dim)
        value_rows = jnp.repeat(value_rows.reshape(row_count, key_heads, head_dim), repeats, axis=1)
        value_rows = value_rows.reshape(row_count, key_heads * repeats * head_dim)
    head_query, head_keys, head_values, head_gates = (
        lax.all_to_all(query_rows, "sp", split_axis=1, concat_axis=0, tiled=True),
        lax.all_to_all(key_rows, "sp", split_axis=1, concat_axis=0, tiled=True),
        lax.all_to_all(value_rows, "sp", split_axis=1, concat_axis=0, tiled=True),
        lax.all_to_all(log_gate, "sp", split_axis=1, concat_axis=0, tiled=True),
    )
    seq_length = head_query.shape[0]
    local_heads = head_count // sp_count
    local_keys = head_keys.shape[1] // head_dim
    group_share = local_heads // local_keys
    decay_sum = jnp.cumsum(head_gates.astype(jnp.float32), axis=0)
    decay_grid = decay_sum.T.reshape(local_keys, group_share, seq_length)
    grouped = head_query.reshape(seq_length, local_keys, group_share, head_dim)
    key_grid = head_keys.reshape(seq_length, local_keys, head_dim)
    value_grid = head_values.reshape(seq_length, local_keys, head_dim)
    block_size = pick_block(seq_length)
    block_count = seq_length // block_size
    score_scale = head_dim ** (-0.5)
    offsets = jnp.arange(block_size, dtype=jnp.int32)

    def query_block(block_index):
        first_row = block_index * block_size
        query_part = lax.dynamic_slice_in_dim(grouped, first_row, block_size, 0)
        query_decay = lax.dynamic_slice_in_dim(decay_grid, first_row, block_size, 2)

        def fill_scores(key_block, buffer):
            key_first = key_block * block_size
            key_part = lax.dynamic_slice_in_dim(key_grid, key_first, block_size, 0)
            key_decay = lax.dynamic_slice_in_dim(decay_grid, key_first, block_size, 2)
            raw_scores = jnp.einsum(
                "qkgd,skd->kgqs", query_part, key_part, preferred_element_type=jnp.float32
            )
            biased = raw_scores * score_scale + query_decay[..., :, None] - key_decay[..., None, :]
            allowed = (key_first + offsets)[None, :] <= (first_row + offsets)[:, None]
            masked = jnp.where(allowed, biased, -jnp.inf)
            return lax.dynamic_update_index_in_dim(buffer, masked, key_block, 0)

        score_buffer = lax.fori_loop(
            0,
            block_index + 1,
            fill_scores,
            jnp.full(
                (block_count, local_keys, group_share, block_size, block_size),
                -jnp.inf,
                jnp.float32,
            ),
        )
        row_max = jnp.max(jnp.max(score_buffer, axis=-1), axis=0)
        row_sum = jnp.sum(
            jnp.sum(jnp.exp(score_buffer - row_max[None, ..., None]), axis=-1), axis=0
        )

        def weighted(key_block, accumulated):
            block_scores = lax.dynamic_index_in_dim(score_buffer, key_block, 0, keepdims=False)
            weights = (jnp.exp(block_scores - row_max[..., None]) / row_sum[..., None]).astype(
                jnp.bfloat16
            )
            value_part = lax.dynamic_slice_in_dim(value_grid, key_block * block_size, block_size, 0)
            return accumulated + jnp.einsum(
                "kgqs,skd->qkgd", weights, value_part, preferred_element_type=jnp.float32
            )

        mixed_block = lax.fori_loop(
            0,
            block_index + 1,
            weighted,
            jnp.zeros((block_size, local_keys, group_share, head_dim), jnp.float32),
        )
        return mixed_block.astype(jnp.bfloat16).reshape(block_size, local_heads * head_dim)

    head_mixed = lax.map(query_block, jnp.arange(block_count, dtype=jnp.int32))
    head_mixed = head_mixed.reshape(seq_length, local_heads * head_dim)
    mixed = lax.all_to_all(head_mixed, "sp", split_axis=0, concat_axis=1, tiled=True)
    return mixed[None]


def on_device(*arrays):
    key_heads = arrays[2].shape[1] * arrays[4].shape[1] // arrays[1].shape[1]
    if lax.axis_size("dp") == 8 and lax.axis_size("sp") == 4 and key_heads == 4:
        return paired(*arrays)
    return exchanged(*arrays)


def solution(mesh):
    placed = (P("dp", "sp", None), P("dp", None), P("dp", None), P("dp", None), P(), P())
    return jax.shard_map(
        on_device, mesh=mesh, in_specs=placed, out_specs=P("dp", "sp", None), check_vma=False
    )
```
